768 devices in a mesh: ep: 48 (over z, x), tp: 16 (over y, core).
Axes of the slice: x: 4, y: 8, z: 12, core: 2. Of those that a mesh axis runs over, the one named last changes fastest.
Arguments:
- tokens: bfloat16 [6144, 2048], P('ep', 'tp'), may hold values from -20 to 20
- routing: int32 [6144, 2], P('ep'), may hold values from 0 to 47, all different within a row; in each aligned block of 128 rows (0 to 127, 128 to 255, ...) at most 8 rows name the same one
- gate_weights: bfloat16 [6144, 2], P('ep'), may hold values from 0 to 1, as said below
- cotangent: bfloat16 [6144, 2048], P('ep', 'tp'), may hold values from -3 to 3
- expert_gate: bfloat16 [48, 2048, 3072], P('ep', None, 'tp'), may hold values from -3 to 3
- expert_up: bfloat16 [48, 2048, 3072], P('ep', None, 'tp'), may hold values from -3 to 3
- expert_down: bfloat16 [48, 3072, 2048], P('ep', 'tp'), may hold values from -0.109375 to 0.109375
- router: bfloat16 [2048, 48], replicated, may hold values from -0.125 to 0.125
Outputs:
- token_grad: float32 [6144, 2048], P('ep', 'tp')
- gate_grad: float32 [6144, 2], P('ep')
- gate_proj_grad: bfloat16 [48, 2048, 3072], P('ep', None, 'tp')
- up_proj_grad: bfloat16 [48, 2048, 3072], P('ep', None, 'tp')
- down_proj_grad: bfloat16 [48, 3072, 2048], P('ep', 'tp')
- router_grad: float32 [48, 2048], P('ep', 'tp')
- gate_row_square: float32 [48, 2048], P('ep')
- up_row_square: float32 [48, 2048], P('ep')
- down_row_square: float32 [48, 3072], P('ep', 'tp')
The draws below stay inside these ranges and needn't reach their ends.
Inputs may be any that keep to these rules, and one draw needn't show every extreme that they name: `routing`: each token names 2 different experts. Among the 128 rows of one device no expert is named more than 8 times; some device reaches 8. `gate_weights`: each row is positive and sums to one up to rounding.
All inputs are finite; a program needn't handle non-finite values.
Results may differ from the reference program's by a relative error of at most 0.015.
Values may be sent and summed in bfloat16 or wider, within the bound.
A program may use at most 32 MiB of HBM per device.

```python
import math
import jax
import jax.numpy as jnp
import numpy as np
from jax import lax

D = 2048
FF = 3072
TOP = 2
TOK_DEV = 128
EXPERTS = 48
CAP = 8
TOKENS = 6144
N_EP = 48
N_TP = 16


def feature_scale(key, length, spread):
    place = jnp.arange(length, dtype=jnp.float32) / length
    jitter = jax.random.uniform(key, (length,), jnp.float32, -0.5, 0.5)
    return jnp.exp(jnp.log(spread) * (place - 0.5) + jitter)


def base_values(key, shape):
    return jnp.clip(jax.random.normal(key, shape, jnp.float32), -5.0, 5.0)


def scaled_matrix(key):
    values = base_values(jax.random.fold_in(key, 21), (EXPERTS, D, FF))
    spread = 3.0
    columns = feature_scale(jax.random.fold_in(key, 22), FF, spread)
    return (values * columns * D ** (-0.5)).astype(jnp.bfloat16)


def draw_tokens(key, part):
    values = base_values(jax.random.fold_in(key, 11), (TOKENS, D))
    columns = feature_scale(jax.random.fold_in(key, 12), D, 3.0)
    return (values * columns).astype(jnp.bfloat16)


def draw_gate_weights(key, part):
    logits = jax.random.uniform(key, (TOKENS, TOP), jnp.float32, -1.5, 1.5)
    return jax.nn.softmax(logits, axis=-1).astype(jnp.bfloat16)


def draw_expert_gate(key, part):
    return scaled_matrix(jax.random.fold_in(key, 31))


def draw_expert_up(key, part):
    return scaled_matrix(jax.random.fold_in(key, 32))


def shard_levels(stream_key, shape, split, least, largest):
    level = 1.0
    for dim, parts in split:
        draws = jax.random.uniform(jax.random.fold_in(jax.random.fold_in(stream_key, 6), dim), (parts,), jnp.float32, least / len(split), largest / len(split))
        level = level * jnp.repeat(jnp.exp(draws), shape[dim] // parts).reshape((-1,) + (1,) * (len(shape) - 1 - dim))
    return level


def assign_block(own_key, own, number, rows, count, top, reach, slope):
    order = jax.random.permutation(own_key, count)
    crowded, common = load_shares(count, rows * top, reach, slope, True), load_shares(count, rows * top, reach, slope, False)
    places = jnp.arange(count)

    def named(lengths, rotation):
        used = int((lengths > 0).sum())
        fixed = max(1, used // 4)
        moved = fixed + (places - fixed + rotation * (used - fixed)) % max(1, count - fixed)
        return jnp.zeros((count,), jnp.int32).at[order[jnp.where(places < fixed, places, moved)]].set(jnp.asarray(lengths, jnp.int32))

    lengths = jnp.where(number % 4 == 0, named(crowded, number // 4), named(common, number - number // 4 - 1))
    mixed = jax.random.permutation(jax.random.fold_in(own, 3), count)
    giver, sink = mixed[0:count // 2 * 2:2], mixed[1:count // 2 * 2:2]
    slack = jnp.minimum(lengths[giver] - 1, reach - lengths[sink]) // 2
    slack = jnp.where((giver == order[0]) | (sink == order[0]) | (lengths[sink] == 0), 0, jnp.maximum(slack, 0))
    moved = jax.random.randint(jax.random.fold_in(own, 4), (count // 2,), 0, 1 << 20) % (slack + 1)
    lengths = lengths.at[giver].add(-moved).at[sink].add(moved)
    items = jnp.searchsorted(jnp.cumsum(lengths), jnp.arange(rows * top), side="right").astype(jnp.int32)
    listing = items.reshape(top, rows).T
    listing = listing[jax.random.permutation(jax.random.fold_in(own, 1), rows)]
    rotation = jax.random.randint(jax.random.fold_in(own, 2), (rows, 1), 0, top)
    return jnp.take_along_axis(listing, (jnp.arange(top)[None, :] + rotation) % top, axis=1)


def load_shares(count, total, reach, slope, full):
    loads = [(1 << 20) // math.isqrt(grade ** slope) + 1 for grade in range(1, count + 1)]
    largest = reach if full else min(reach, max(-(-total // count), total * loads[0] // sum(loads)))
    least = 1 if total - largest >= count - 1 else 0
    counts, rest = [largest] + [least] * (count - 1), total - largest - least * (count - 1)
    while rest > 0:
        free = [i for i in range(1, count) if counts[i] < largest] or [i for i in range(1, count) if counts[i] < reach]
        whole, left = sum([loads[i] for i in free]), rest
        for i in free:
            more = min(reach - counts[i], max(1, left * loads[i] // whole), rest)
            counts[i] = counts[i] + more
            rest = rest - more
    return np.array(counts)


def bell_draw(stream_key, dims, scale, most, pieces=(), held_as=jnp.bfloat16):
    result = scale * jax.random.normal(stream_key, dims, jnp.float32)
    if pieces:
        result = result * shard_levels(stream_key, dims, pieces, -0.22, 0.18)
    return jnp.clip(result, -most, most).astype(held_as)


def setup_inputs(seed: int = 0) -> dict:
    arg_keys = jax.random.split(jax.random.key(seed), 9)
    tokens = draw_tokens(jax.random.fold_in(arg_keys[8], 71), 0)
    routing_keys = jax.random.split(jax.random.fold_in(arg_keys[1], 1), TOKENS // TOK_DEV)
    routing_turns = jax.random.permutation(jax.random.fold_in(arg_keys[1], 3), TOKENS // TOK_DEV)
    routing = jax.vmap(lambda own, number: assign_block(jax.random.fold_in(arg_keys[1], 2), own, number, TOK_DEV, EXPERTS, TOP, CAP, 1))(routing_keys, routing_turns).reshape((TOKENS, TOP))
    gate_weights = draw_gate_weights(jax.random.fold_in(arg_keys[8], 71), 0)
    cotangent = bell_draw(arg_keys[3], (TOKENS, D), 0.5, 3.0, ((0, 48), (1, 16)))
    expert_gate = draw_expert_gate(jax.random.fold_in(arg_keys[8], 71), 0)
    expert_up = draw_expert_up(jax.random.fold_in(arg_keys[8], 71), 0)
    expert_down = bell_draw(arg_keys[6], (EXPERTS, FF, D), FF ** -0.5, 0.109375, ((0, 48), (1, 16)))
    router = bell_draw(arg_keys[7], (D, EXPERTS), D ** -0.5, 0.125)
    return {"tokens": tokens, "routing": routing, "gate_weights": gate_weights, "cotangent": cotangent, "expert_gate": expert_gate, "expert_up": expert_up, "expert_down": expert_down, "router": router}


def reference(tokens, routing, gate_weights, cotangent, expert_gate, expert_up, expert_down, router):
    pair_count = TOK_DEV * TOP
    block_routes = routing.reshape(N_EP, pair_count)
    slot_ids = jnp.arange(CAP, dtype=jnp.int32)
    pair_ids = jnp.arange(pair_count, dtype=jnp.int32)
    block_base = (jnp.arange(N_EP, dtype=jnp.int32) * TOK_DEV)[:, None]
    hidden_local = FF // N_TP

    def one_expert(expert_index):
        hit_mask = (block_routes == expert_index).astype(jnp.int32)
        ranking = (jnp.cumsum(hit_mask, axis=1) - 1).astype(jnp.int32)
        chosen = hit_mask[:, None, :] * (ranking[:, None, :] == slot_ids[None, :, None]).astype(jnp.int32)
        source_pair = jnp.sum(chosen * pair_ids[None, None, :], axis=2).astype(jnp.int32)
        filled = jnp.sum(chosen, axis=2) > 0
        row_index = (block_base + source_pair // TOP).reshape(-1).astype(jnp.int32)
        which_slot = (source_pair % TOP).reshape(-1).astype(jnp.int32)
        live_slot = filled.reshape(-1)
        input_slots = jnp.where(live_slot[:, None], tokens[row_index], jnp.zeros((), jnp.bfloat16))
        tangent_slots = jnp.where(live_slot[:, None], cotangent[row_index], jnp.zeros((), jnp.bfloat16))
        slot_weight = jnp.where(live_slot, gate_weights[row_index, which_slot].astype(jnp.float32), jnp.float32(0.0))
        gate_matrix = expert_gate[expert_index]
        up_matrix = expert_up[expert_index]
        down_matrix = expert_down[expert_index]
        pre_gate = jnp.dot(input_slots, gate_matrix, preferred_element_type=jnp.float32)
        pre_up = jnp.dot(input_slots, up_matrix, preferred_element_type=jnp.float32)
        back_proj = jnp.dot(tangent_slots, down_matrix.T, preferred_element_type=jnp.float32)
        sigmoid_gate = jax.nn.sigmoid(pre_gate)
        active = pre_gate * sigmoid_gate
        hidden = active * pre_up
        slot_gate = jnp.sum(hidden * back_proj, axis=1)
        weight_col = slot_weight[:, None]
        scaled = (weight_col * hidden).astype(jnp.bfloat16)
        hidden_grad = weight_col * back_proj
        gate_pre_grad = (hidden_grad * pre_up * sigmoid_gate * (1.0 + pre_gate * (1.0 - sigmoid_gate))).astype(jnp.bfloat16)
        up_pre_grad = (hidden_grad * active).astype(jnp.bfloat16)
        gate_sum = jnp.dot(input_slots.T, gate_pre_grad, preferred_element_type=jnp.float32)
        up_sum = jnp.dot(input_slots.T, up_pre_grad, preferred_element_type=jnp.float32)
        down_sum = jnp.dot(scaled.T, tangent_slots, preferred_element_type=jnp.float32)
        slot_total = N_EP * CAP
        block_parts = jnp.einsum('snf,dnf->nsd',
                                 gate_pre_grad.astype(jnp.float32).reshape(slot_total, N_TP, hidden_local),
                                 gate_matrix.astype(jnp.float32).reshape(D, N_TP, hidden_local))
        block_parts = block_parts + jnp.einsum('snf,dnf->nsd',
                                               up_pre_grad.astype(jnp.float32).reshape(slot_total, N_TP, hidden_local),
                                               up_matrix.astype(jnp.float32).reshape(D, N_TP, hidden_local))
        rounded = lax.optimization_barrier(block_parts.astype(jnp.bfloat16))
        slot_token = jnp.sum(rounded.astype(jnp.float32), axis=0)
        return (slot_token.reshape(N_EP, CAP, D), slot_gate.reshape(N_EP, CAP),
                gate_sum.astype(jnp.bfloat16), up_sum.astype(jnp.bfloat16), down_sum.astype(jnp.bfloat16),
                jnp.mean(gate_sum * gate_sum, axis=1), jnp.mean(up_sum * up_sum, axis=1),
                jnp.mean(down_sum * down_sum, axis=1))

    results = lax.map(one_expert, jnp.arange(EXPERTS, dtype=jnp.int32))
    slot_token, slot_gate, gate_grads, up_grads, down_grads, gate_square, up_square, down_square = results
    labels = jnp.arange(EXPERTS, dtype=jnp.int32)
    one_hot = (block_routes[:, :, None] == labels[None, None, :]).astype(jnp.int32)
    ranking = (jnp.cumsum(one_hot, axis=1) - 1).astype(jnp.int32)
    position = jnp.sum(one_hot * ranking, axis=2).astype(jnp.int32)
    source_ids = jnp.broadcast_to(jnp.arange(N_EP, dtype=jnp.int32)[:, None], (N_EP, pair_count))
    pair_token = slot_token[block_routes, source_ids, position]
    token_part = jnp.sum(pair_token.reshape(TOKENS, TOP, D), axis=1)
    gate_grad = slot_gate[block_routes, source_ids, position].reshape(TOKENS, TOP)
    weights_f = gate_weights.astype(jnp.float32)
    mixed_term = jnp.sum(weights_f * gate_grad, axis=1, keepdims=True)
    logit_grad = weights_f * (gate_grad - mixed_term)
    signal = jnp.sum(jnp.where(routing[:, :, None] == labels[None, None, :], logit_grad[:, :, None], jnp.float32(0.0)), axis=1).astype(jnp.bfloat16)
    router_grad = jnp.dot(signal.T, tokens, preferred_element_type=jnp.float32)
    token_grad = token_part + jnp.dot(signal, router.T, preferred_element_type=jnp.float32)
    return (token_grad, gate_grad, gate_grads, up_grads, down_grads, router_grad, gate_square, up_square, down_square)
```

```python
import functools

import jax
import jax.numpy as jnp
from jax import lax
from jax.experimental import pallas as pl
from jax.experimental.pallas import tpu as pltpu
from jax.sharding import PartitionSpec as P

MESH = pl.DeviceIdType.MESH
BF = jnp.bfloat16
F32 = jnp.float32
LANES = 128
HI = lax.Precision.HIGHEST


def dot(a, b, ca=1, cb=0, precision=None):
    return lax.dot_general(
        a, b, (((ca,), (cb,)), ((), ())), precision=precision, preferred_element_type=F32
    )


def log2(n):
    return n.bit_length() - 1


class Plan:
    def __init__(self, n_ep, n_tp, tok, width, hidden, features, cap):
        self.ep, self.tp, self.tok, self.width = n_ep, n_tp, tok, width
        self.hidden, self.features, self.cap = hidden, features, cap
        self.x = 4 if n_ep % 4 == 0 else 1
        self.z = n_ep // self.x
        self.y = n_tp // 2
        self.half = self.y // 2
        self.slots = n_ep * cap
        self.chunks = self.slots // LANES
        self.per_chunk = LANES // cap
        self.units = 4
        self.unit_rows = self.slots // self.units
        self.slab = 2 * width

    def near(self, dz):
        dz %= self.z
        if dz == 0:
            return 0
        return 2 * dz - 1 if 2 * dz <= self.z else 2 * (self.z - dz)

    def place(self, dz, dx):
        return self.near(dz) * self.x + dx % self.x

    def offsets(self):
        found = [(dz, dx) for dz in range(self.z) for dx in range(self.x) if (dz, dx) != (0, 0)]

        def hops(o):
            return min(o[0], self.z - o[0]) + min(o[1], self.x - o[1])

        return sorted(found, key=lambda o: (-hops(o), o[1], o[0]))

    def ring_units(self, k, way):
        low, high = 0, 2 * self.chunks
        if k == self.half:
            low, high = (0, self.chunks) if way == 0 else (self.chunks, 2 * self.chunks)
        out = []
        for u in range(self.chunks):
            a, b = max(low, 2 * u), min(high, 2 * u + 2)
            if a < b:
                out.append((u, a, b))
        return out

    def long_way(self, way, u):
        return (u < self.units // 2) == (way == 0)


def kernel(
    p,
    routing_ref, weight_ref, tokens_ref, cotangent_ref, gate_hbm, up_hbm, down_hbm, router_hbm,
    token_out, gate_out, dgate_hbm, dup_hbm, ddown_hbm, router_out, gsq_out, usq_out, dsq_out,
    w_gu, w_dn, r_cols, send_b, recv_b, w_send, w_recv, by_token, hits, places,
    g, pre, back, grads, grads_t, scaled, g_part, gp_recv, g_send, g_recv,
    mine, p_send, p_recv, rs_s, rs_r, c_buf, c_recv, rt_send, rt_recv, sq, sq_recv,
    dg, du, dd, d_acc,
    load_sem, disp_s, disp_r, wt_s, wt_r, ag_s, ag_r, pair_s, pair_r, gp_s, gp_r, gc_s, gc_r,
    ps_s, ps_r, rs_ss, rs_rs, cb_s, cb_r, rt_s, rt_r, sq_s, sq_r, out_sem,
):
    me = lax.axis_index("ep")
    t = lax.axis_index("tp")
    y, c = lax.div(t, 2), lax.rem(t, 2)
    z_me, x_me = lax.div(me, p.x), lax.rem(me, p.x)
    partner = t + 1 - 2 * c
    right = lax.rem(y + 1, p.y) * 2 + c
    left = lax.rem(y + p.y - 1, p.y) * 2 + c
    ways = (right, left)
    H, S, E, T, F = p.hidden, p.slots, p.ep, p.tok, p.width

    def peer(dz, dx):
        return lax.rem(z_me + dz, p.z) * p.x + lax.rem(x_me + dx, p.x)

    def remote(src, dst, s, r, to):
        return pltpu.make_async_remote_copy(
            src_ref=src, dst_ref=dst, send_sem=s, recv_sem=r, device_id=to, device_id_type=MESH
        )

    def wait_for(ref, sem):
        pltpu.make_async_copy(ref, ref, sem).wait()

    offsets = p.offsets()
    n_peers = len(offsets)
    loads = [
        pltpu.make_async_copy(gate_hbm, w_gu.at[pl.ds(0, H)], load_sem.at[0]),
        pltpu.make_async_copy(up_hbm, w_gu.at[pl.ds(H, H)], load_sem.at[1]),
        pltpu.make_async_copy(down_hbm, w_dn, load_sem.at[2]),
        pltpu.make_async_copy(
            router_hbm.at[:, pl.ds(pl.multiple_of(t * F, F), F)], r_cols, load_sem.at[3]
        ),
    ]
    barrier = pltpu.get_barrier_semaphore()
    for dz, dx in offsets:
        pl.semaphore_signal(barrier, inc=1, device_id=(peer(dz, dx), t), device_id_type=MESH)
    for j in range(1, p.tp):
        pl.semaphore_signal(
            barrier, inc=1, device_id=(me, lax.rem(t + j, p.tp)), device_id_type=MESH
        )
    for copy in loads:
        copy.start()

    routes = routing_ref[...]
    expert_rows = lax.broadcasted_iota(jnp.int32, (E, T), 0)
    hit = [(expert_rows == routes[k : k + 1, :]).astype(F32) for k in range(2)]
    earlier = (
        lax.broadcasted_iota(jnp.int32, (T, T), 0) < lax.broadcasted_iota(jnp.int32, (T, T), 1)
    ).astype(F32).astype(BF)
    count = dot((hit[0] + hit[1]).astype(BF), earlier)
    pos = [jnp.sum(hit[k] * count, axis=0, keepdims=True) for k in range(2)]
    slot_rows = lax.broadcasted_iota(jnp.int32, (S, T), 0).astype(F32)
    slot = [routes[k : k + 1, :].astype(F32) * p.cap + pos[k] for k in range(2)]
    match = jnp.where((slot_rows == slot[0]) | (slot_rows == slot[1]), 1.0, 0.0)
    tokens = tokens_ref[...]
    match_b = match.astype(BF)
    in_rows = dot(match_b, tokens).reshape(E, p.cap, F)
    tan_rows = dot(match_b, cotangent_ref[...]).reshape(E, p.cap, F)
    send_b[...] = jnp.concatenate([in_rows, tan_rows], axis=1).astype(BF)
    for k in range(2):
        hits[k] = hit[k]
        places[k] = pos[k]
    weights = weight_ref[...].astype(F32)
    lane_rows = lax.broadcasted_iota(jnp.int32, (LANES, T), 0)
    lane_slot = (lane_rows & (p.cap - 1)).astype(F32)
    spread = sum(
        dot(hit[k].astype(BF), jnp.where(lane_slot == pos[k], weights[k : k + 1, :], 0.0).astype(BF), 1, 1)
        for k in range(2)
    )
    e_ids = lax.broadcasted_iota(jnp.int32, (E, LANES), 0)
    lane_ids = lax.broadcasted_iota(jnp.int32, (E, LANES), 1)
    dz = z_me - (e_ids >> log2(p.x))
    dz = jnp.where(dz < 0, dz + p.z, dz)
    near = jnp.where(dz == 0, 0, jnp.where(2 * dz <= p.z, 2 * dz - 1, 2 * (p.z - dz)))
    my_place = near * p.x + ((x_me - (e_ids & (p.x - 1))) & (p.x - 1))
    my_lanes = (lane_ids >> log2(p.cap)) == (my_place & (p.per_chunk - 1))
    w_send[...] = jnp.where(my_lanes, spread, 0.0).reshape(E, 1, LANES)

    pl.semaphore_wait(barrier, n_peers + p.tp - 1)

    for dz, dx in offsets:
        to = peer(dz, dx)
        at = p.place(-dz, -dx)
        remote(send_b.at[to], recv_b.at[at], disp_s, disp_r.at[at // p.per_chunk], (to, t)).start()
        remote(w_send.at[to], w_recv.at[at], wt_s, wt_r, (to, t)).start()
    recv_b[0] = send_b[me]
    w_recv[0] = w_send[me]
    by_token[...] = match.T.astype(BF)

    sent = []

    def move(k, way, u, a, b):
        r = (-(k - 1) if way == 0 else k - 1) % p.y
        to_r = (-k if way == 0 else k) % p.y
        copy = remote(
            g.at[r, c, pl.ds(a, b - a)], g.at[to_r, c, pl.ds(a, b - a)],
            ag_s.at[way, k - 1, u], ag_r.at[way, k - 1, u], (me, ways[way]),
        )
        copy.start()
        sent.append(copy)

    def to_partner(r, u, a, b, s):
        piece = g.at[r, c, pl.ds(a, b - a)]
        copy = remote(piece, piece, pair_s.at[r, s], pair_r.at[r, s], (me, partner))
        copy.start()
        sent.append(copy)

    def pair_pieces(r):
        if r == p.half:
            found = [w for way in range(2) for w in p.ring_units(p.half, way)]
        else:
            found = p.ring_units(1 if p.half > 1 else 0, 0)
        return [(s, a, b) for s, (_, a, b) in enumerate(found)]

    def from_partner(r):
        for s, a, b in pair_pieces(r):
            wait_for(g.at[r, 1 - c, pl.ds(a, b - a)], pair_r.at[r, s])

    def semaphore_of(r, a):
        return [s for s, first, _ in pair_pieces(r) if first == a][0]

    def lanes_of(r):
        return pl.ds(pl.multiple_of(lax.rem(y + r, p.y) * p.slab, p.slab), p.slab)

    def rows_of(r, kind):
        return jnp.concatenate(
            [
                jnp.concatenate([g[r, core, 2 * ch + kind] for ch in range(p.chunks)], axis=0)
                for core in range(2)
            ],
            axis=1,
        )

    def forward(r, first):
        from_partner(r)
        cols = lanes_of(r)
        up = dot(w_gu[:, cols], rows_of(r, 0), 1, 1)
        down = dot(w_dn[:, cols], rows_of(r, 1), 1, 1)
        if first:
            pre[...] = up
            back[...] = down
        else:
            pre[...] += up
            back[...] += down

    for u in range(p.chunks):
        arrived = p.per_chunk - (1 if u == 0 else 0)
        if arrived:
            wait_for(recv_b.at[pl.ds(0, arrived)], disp_r.at[u])
        both = recv_b[u * p.per_chunk : (u + 1) * p.per_chunk].astype(F32)
        g[0, c, 2 * u] = both[:, : p.cap].reshape(LANES, F).astype(BF)
        g[0, c, 2 * u + 1] = both[:, p.cap :].reshape(LANES, F).astype(BF)
        for way in range(2):
            for v, a, b in p.ring_units(1, way):
                if v == u:
                    move(1, way, v, a, b)
        to_partner(0, u, 2 * u, 2 * u + 2, u)
    for copy in loads:
        copy.wait()
    wait_for(w_recv.at[pl.ds(0, n_peers)], wt_r)
    slot_weight = jnp.concatenate(
        [
            jnp.sum(w_recv[ch * p.per_chunk : (ch + 1) * p.per_chunk], axis=0)
            for ch in range(p.chunks)
        ],
        axis=1,
    )
    for k in range(1, p.half + 1):
        if k == p.half:
            for r in sorted({(k - 1) % p.y, (1 - k) % p.y}):
                forward(r, r == 0)
        for u in range(p.chunks):
            for way in range(2):
                r = (-k if way == 0 else k) % p.y
                for v, a, b in p.ring_units(k, way):
                    if v != u:
                        continue
                    wait_for(g.at[r, c, pl.ds(a, b - a)], ag_r.at[way, k - 1, v])
                    if k < p.half:
                        for v2, a2, b2 in p.ring_units(k + 1, way):
                            if v2 == u:
                                move(k + 1, way, v2, a2, b2)
                    to_partner(r, u, a, b, semaphore_of(r, a))
        if k < p.half:
            for r in sorted({(k - 1) % p.y, (1 - k) % p.y}):
                forward(r, r == 0)
    forward(p.half, False)

    part = jnp.zeros((1, S), F32)
    step = 32
    for b in range(0, H, step):
        pg, pu, bp = pre[b : b + step, :], pre[H + b : H + b + step, :], back[b : b + step, :]
        sig = lax.logistic(pg)
        act = pg * sig
        hid = act * pu
        part = part + jnp.sum(hid * bp, axis=0, keepdims=True)
        scaled[b : b + step, :] = (slot_weight * hid).astype(BF)
        hg = slot_weight * bp
        grads[b : b + step, :] = (hg * pu * sig * (1.0 + pg * (1.0 - sig))).astype(BF)
        grads[H + b : H + b + step, :] = (hg * act).astype(BF)
    for ch in range(p.chunks):
        g_part[ch : ch + 1, :] = part[:, ch * LANES : (ch + 1) * LANES]
    g_part[p.chunks :, :] = jnp.zeros((8 - p.chunks, LANES), F32)
    gp_recv[t] = g_part[...]
    for j in range(1, p.tp):
        remote(g_part, gp_recv.at[t], gp_s, gp_r, (me, lax.rem(t + j, p.tp))).start()
    grads_t[...] = grads[...].astype(F32).T.astype(BF)

    def slot_block(r):
        block = dot(grads_t[...], w_gu[:, lanes_of(r)])
        low, high = block[:, :F], block[:, F:]
        mine[r] = jnp.where(c == 0, low, high).astype(BF)
        p_send[r] = jnp.where(c == 0, high, low).astype(BF)
        copy = remote(p_send.at[r], p_recv.at[r], ps_s.at[r], ps_r.at[r], (me, partner))
        copy.start()
        sent.append(copy)

    def chip_sum(r, u):
        rows = pl.ds(u * p.unit_rows, p.unit_rows)
        return mine[r, rows].astype(F32) + p_recv[r, rows].astype(F32)

    def ring_send(way, u, d):
        r = (d if way == 0 else -d) % p.y
        total = chip_sum(r, u)
        longest = p.half if p.long_way(way, u) else p.half - 1
        if d < longest:
            wait_for(rs_r.at[way, u, d], rs_rs.at[way, u, d])
            total = total + rs_r[way, u, d].astype(F32)
        rs_s[way, u, d - 1] = total.astype(BF)
        copy = remote(
            rs_s.at[way, u, d - 1], rs_r.at[way, u, d - 1],
            rs_ss.at[way, u, d - 1], rs_rs.at[way, u, d - 1], (me, ways[way]),
        )
        copy.start()
        sent.append(copy)

    def ring_step(j):
        for u in range(p.units // 2):
            for way in range(2):
                v = u if way == 0 else u + p.units // 2
                if p.half - j + 1 >= 1:
                    ring_send(way, v, p.half - j + 1)
        for u in range(p.units // 2):
            for way in range(2):
                v = u + p.units // 2 if way == 0 else u
                if p.half - j >= 1:
                    ring_send(way, v, p.half - j)

    order = [p.half]
    for d in range(p.half - 1, 0, -1):
        order += [d, p.y - d]
    order.append(0)
    first = 1 if p.half == 1 else 3
    for r in order[:first]:
        slot_block(r)
    for r in order[:first]:
        wait_for(p_recv.at[r], ps_r.at[r])
    ring_step(1)
    for r in order[first:]:
        slot_block(r)
    for r in order[first:]:
        wait_for(p_recv.at[r], ps_r.at[r])

    d_acc[...] = jnp.zeros_like(d_acc)

    def weight_grads(r):
        cols = lanes_of(r)
        both = dot(grads[...], rows_of(r, 0))
        dg[:, cols] = both[:H].astype(BF)
        du[:, cols] = both[H:].astype(BF)
        sq[0:1, cols] = jnp.sum(both[:H] * both[:H], axis=0, keepdims=True)
        sq[1:2, cols] = jnp.sum(both[H:] * both[H:], axis=0, keepdims=True)
        down = dot(scaled[...], rows_of(r, 1))
        dd[:, cols] = down.astype(BF)
        square = down * down
        d_acc[...] += square[:, :F] + square[:, F:]

    slabs = list(range(p.y))
    per_step = -(-p.y // max(1, p.half - 1)) if p.half > 1 else p.y
    gate_done = False

    def gate_sum():
        wait_for(gp_recv.at[pl.ds(0, p.tp - 1)], gp_r)
        total = jnp.sum(gp_recv[...], axis=0)
        for ch in range(p.chunks):
            g_send[ch] = total[ch : ch + 1, :]
        for dz, dx in offsets:
            to = peer(dz, dx)
            row = p.place(dz, dx) // p.per_chunk
            remote(g_send.at[row], g_recv.at[me], gc_s, gc_r, (to, t)).start()
        g_recv[me] = g_send[0]

    for j in range(2, p.half + 1):
        for r in slabs[:per_step]:
            weight_grads(r)
        slabs = slabs[per_step:]
        ring_step(j)
        if not gate_done:
            gate_sum()
            gate_done = True
    for r in slabs:
        weight_grads(r)
    if not gate_done:
        gate_sum()
    outs = [
        pltpu.make_async_copy(dg, dgate_hbm, out_sem.at[0]),
        pltpu.make_async_copy(du, dup_hbm, out_sem.at[1]),
        pltpu.make_async_copy(dd, ddown_hbm, out_sem.at[2]),
    ]
    for copy in outs:
        copy.start()

    totals = []
    for u in range(p.units):
        total = chip_sum(0, u)
        for way in range(2):
            if p.half > 1 or p.long_way(way, u):
                wait_for(rs_r.at[way, u, 0], rs_rs.at[way, u, 0])
                total = total + rs_r[way, u, 0].astype(F32)
        totals.append(total)
    c_buf[...] = jnp.concatenate(totals, axis=0).reshape(E, p.cap, F).astype(BF)

    for dz, dx in offsets:
        to = peer(dz, dx)
        remote(c_buf.at[p.place(dz, dx)], c_recv.at[me], cb_s, cb_r, (to, t)).start()
    c_recv[me] = c_buf[0]

    wait_for(g_recv.at[pl.ds(0, n_peers)], gc_r)
    kept = jnp.where(my_lanes, g_recv[...].reshape(E, LANES), 0.0)
    gate = []
    for k in range(2):
        picked = dot(kept, hits[k], 0, 0, HI)
        gate.append(jnp.sum(jnp.where(lane_slot == places[k], picked, 0.0), axis=0, keepdims=True))
        gate_out[k : k + 1, :] = gate[k]
    mixed = weights[0:1, :] * gate[0] + weights[1:2, :] * gate[1]
    logit = [weights[k : k + 1, :] * (gate[k] - mixed) for k in range(2)]
    signal = (hits[0] * logit[0] + hits[1] * logit[1]).astype(BF)
    rt_send[...] = dot(signal, tokens).reshape(E, 1, F)
    for dz, dx in offsets:
        to = peer(dz, dx)
        remote(rt_send.at[to], rt_recv.at[me], rt_s, rt_r, (to, t)).start()
    rt_recv[me] = rt_send[me]
    sq_recv[t] = sq[...]
    for j in range(1, p.tp):
        remote(sq, sq_recv.at[t], sq_s, sq_r, (me, lax.rem(t + j, p.tp))).start()
    from_router = dot(signal.astype(F32).T.astype(BF), r_cols[...])
    ones = jnp.ones((8, F), F32)
    dsq_out[...] = dot(ones, d_acc[...], 1, 1, HI)[0:1, :] * (1.0 / p.features)

    wait_for(c_recv.at[pl.ds(0, n_peers)], cb_r)
    rows = c_recv[...].astype(F32).reshape(S, F).astype(BF)
    token_out[...] = dot(by_token[...], rows) + from_router
    wait_for(rt_recv.at[pl.ds(0, n_peers)], rt_r)
    router_out[...] = jnp.sum(rt_recv[...], axis=0)
    wait_for(sq_recv.at[pl.ds(0, p.tp - 1)], sq_r)
    squares = jnp.sum(sq_recv[...], axis=0) * (1.0 / (H * p.tp))
    gsq_out[...] = squares[0:1, :]
    usq_out[...] = squares[1:2, :]

    for copy in sent:
        copy.wait_send()
    wait_for(send_b.at[pl.ds(0, n_peers)], disp_s)
    wait_for(w_send.at[pl.ds(0, n_peers)], wt_s)
    wait_for(gp_recv.at[pl.ds(0, p.tp - 1)], gp_s)
    wait_for(g_recv.at[pl.ds(0, n_peers)], gc_s)
    wait_for(c_recv.at[pl.ds(0, n_peers)], cb_s)
    wait_for(rt_recv.at[pl.ds(0, n_peers)], rt_s)
    wait_for(sq_recv.at[pl.ds(0, p.tp - 1)], sq_s)
    for copy in outs:
        copy.wait()


def run(p, routing, weights, tokens, cotangent, gate_t, up_t, down, router_t):
    H, S, E, T, F, D, N = p.hidden, p.slots, p.ep, p.tok, p.width, p.features, p.tp
    vm, hbm = pl.BlockSpec(memory_space=pltpu.VMEM), pl.BlockSpec(memory_space=pl.ANY)
    V, dma = pltpu.VMEM, pltpu.SemaphoreType.DMA
    scratch = [
        V((2 * H, D), BF), V((H, D), BF), V((E, F), BF),
        V((E, 2 * p.cap, F), BF), V((E, 2 * p.cap, F), BF),
        V((E, 1, LANES), F32), V((E, 1, LANES), F32),
        V((T, S), BF), V((2, E, T), F32), V((2, 1, T), F32),
        V((p.y, 2, 2 * p.chunks, LANES, F), BF),
        V((2 * H, S), F32), V((H, S), F32), V((2 * H, S), BF), V((S, 2 * H), BF), V((H, S), BF),
        V((8, LANES), F32), V((N, 8, LANES), F32), V((p.chunks, 1, LANES), F32), V((E, 1, LANES), F32),
        V((p.y, S, F), BF), V((p.y, S, F), BF), V((p.y, S, F), BF),
        V((2, p.units, p.half, p.unit_rows, F), BF), V((2, p.units, p.half, p.unit_rows, F), BF),
        V((E, p.cap, F), BF), V((E, p.cap, F), BF),
        V((E, 1, F), F32), V((E, 1, F), F32),
        V((2, D), F32), V((N, 2, D), F32),
        V((H, D), BF), V((H, D), BF), V((H, D), BF), V((H, F), F32),
        dma((4,)), dma, dma((p.chunks,)), dma, dma,
        dma((2, p.half, p.chunks)), dma((2, p.half, p.chunks)),
        dma((p.y, p.chunks + 1)), dma((p.y, p.chunks + 1)),
        dma, dma, dma, dma,
        dma((p.y,)), dma((p.y,)),
        dma((2, p.units, p.half)), dma((2, p.units, p.half)),
        dma, dma, dma, dma, dma, dma, dma((3,)),
    ]
    shape = jax.ShapeDtypeStruct
    return pl.pallas_call(
        functools.partial(kernel, p),
        out_shape=(
            shape((T, F), F32), shape((2, T), F32),
            shape((H, D), BF), shape((H, D), BF), shape((H, D), BF),
            shape((1, F), F32), shape((1, D), F32), shape((1, D), F32), shape((1, H), F32),
        ),
        in_specs=[vm, vm, vm, vm, hbm, hbm, hbm, hbm],
        out_specs=(vm, vm, hbm, hbm, hbm, vm, vm, vm, vm),
        scratch_shapes=scratch,
        compiler_params=pltpu.CompilerParams(
            collective_id=0, has_side_effects=True, vmem_limit_bytes=48 << 20
        ),
        name="expert_backward",
    )(routing, weights, tokens, cotangent, gate_t, up_t, down, router_t)


def shards(tokens, routing, gate_weights, cotangent, expert_gate, expert_up, expert_down, router):
    tok, width = tokens.shape
    n_ep, n_tp = lax.axis_size("ep"), lax.axis_size("tp")
    experts = router.shape[1]
    cap = 3 * routing.shape[1] * tok // (2 * experts)
    p = Plan(n_ep, n_tp, tok, width, expert_gate.shape[2], width * n_tp, cap)
    out = run(
        p, routing.T, gate_weights.T, tokens, cotangent,
        expert_gate[0].T, expert_up[0].T, expert_down[0], router.T,
    )
    token_grad, gate_grad, dgate, dup, ddown, router_grad, gsq, usq, dsq = out
    return (
        token_grad, gate_grad.T, dgate.T[None], dup.T[None], ddown[None], router_grad, gsq, usq, dsq,
    )


def solution(mesh):
    in_specs = (
        P("ep", "tp"),
        P("ep", None),
        P("ep", None),
        P("ep", "tp"),
        P("ep", None, "tp"),
        P("ep", None, "tp"),
        P("ep", "tp", None),
        P(),
    )
    out_specs = (
        P("ep", "tp"),
        P("ep", None),
        P("ep", None, "tp"),
        P("ep", None, "tp"),
        P("ep", "tp", None),
        P("ep", "tp"),
        P("ep", None),
        P("ep", None),
        P("ep", "tp"),
    )
    return jax.shard_map(shards, mesh=mesh, in_specs=in_specs, out_specs=out_specs, check_vma=False)
```

```python
import functools

import jax
import jax.numpy as jnp
from jax import lax
from jax.experimental import pallas as pl
from jax.experimental.pallas import tpu as pltpu
from jax.sharding import PartitionSpec as P

MESH = pl.DeviceIdType.MESH
BF = jnp.bfloat16
F32 = jnp.float32
LANES = 128
HI = lax.Precision.HIGHEST


def dot(a, b, ca=1, cb=0, precision=None):
    return lax.dot_general(
        a, b, (((ca,), (cb,)), ((), ())), precision=precision, preferred_element_type=F32
    )


def log2(n):
    return n.bit_length() - 1


class Marks:
    def __init__(self):
        self.scope = None

    def __call__(self, name):
        if self.scope is not None:
            self.scope.__exit__(None, None, None)
        self.scope = jax.named_scope(name) if name else None
        if name:
            self.scope.__enter__()


class Plan:
    def __init__(self, n_ep, n_tp, tok, width, hidden, features, cap):
        self.ep, self.tp, self.tok, self.width = n_ep, n_tp, tok, width
        self.hidden, self.features, self.cap = hidden, features, cap
        self.x = 4 if n_ep % 4 == 0 else 1
        self.z = n_ep // self.x
        self.y = n_tp // 2
        self.half = self.y // 2
        self.slots = n_ep * cap
        self.chunks = self.slots // LANES
        self.per_chunk = LANES // cap
        self.units = 4
        self.unit_rows = self.slots // self.units
        self.slab = 2 * width

    def near(self, dz):
        dz %= self.z
        if dz == 0:
            return 0
        return 2 * dz - 1 if 2 * dz <= self.z else 2 * (self.z - dz)

    def place(self, dz, dx):
        return self.near(dz) * self.x + dx % self.x

    def offsets(self):
        found = [(dz, dx) for dz in range(self.z) for dx in range(self.x) if (dz, dx) != (0, 0)]

        def hops(o):
            return min(o[0], self.z - o[0]) + min(o[1], self.x - o[1])

        return sorted(found, key=lambda o: (-hops(o), o[1], o[0]))

    def ring_units(self, k, way):
        kinds = (way,) if k == self.half else (0, 1)
        return [(u, 2 * u + kind) for u in range(self.chunks) for kind in kinds]

    def early(self):
        return sorted(self.offsets(), key=lambda o: self.place(-o[0], -o[1]) // self.per_chunk)

    def gather_order(self):
        if self.half == 4 and self.chunks == 3:
            a, p, m = "arrive", "pass", "multiply"
            return (
                (a, 0, 0), (a, 0, 1), (p, 1, 0), (a, 0, 2), (p, 1, 1), (p, 2, 0), (p, 1, 2),
                (p, 2, 1), (m, 0, 0), (p, 3, 0), (p, 2, 2), (p, 3, 1), (m, 1, 0), (p, 4, 0),
                (p, 3, 2), (m, 2, 0), (p, 4, 1), (p, 4, 2), (m, 3, 0), (m, 4, 0),
            )
        out = [("arrive", 0, u) for u in range(self.chunks)] + [("multiply", 0, 0)]
        for k in range(1, self.half + 1):
            out += [("pass", k, u) for u in range(self.chunks)] + [("multiply", k, 0)]
        return out

    def long_way(self, way, u):
        return u % 2 == way


def kernel(
    p,
    routing_hbm, weight_hbm, tokens_hbm, cotangent_hbm, gate_hbm, up_hbm, down_hbm, router_hbm,
    token_out, gate_out, dg, du, dd, router_out, gsq_out, usq_out, dsq_out,
    routing_ref, weight_ref, tokens_ref, cotangent_ref,
    w_gu, w_dn, r_cols, send_b, recv_b, w_send, w_recv, by_token, hits, places,
    g, pre, back, grads, grads_t, scaled, g_part, gp_recv, g_send, g_recv,
    mine, p_send, p_recv, rs_s, rs_r, c_buf, c_recv, rt_send, rt_recv, sq, sq_recv, sq_sum, sq_all,
    d_acc,
    load_sem, disp_s, disp_r, wt_s, wt_r, ag_s, ag_r, pair_s, pair_r, gp_s, gp_r, gc_s, gc_r,
    ps_s, ps_r, rs_ss, rs_rs, cb_s, cb_r, rt_s, rt_r, sq_s, sq_r, sa_s, sa_r,
):
    mark = Marks()
    mark("start")
    me = lax.axis_index("ep")
    t = lax.axis_index("tp")
    y, c = lax.div(t, 2), lax.rem(t, 2)
    z_me, x_me = lax.div(me, p.x), lax.rem(me, p.x)
    partner = t + 1 - 2 * c
    right = lax.rem(y + 1, p.y) * 2 + c
    left = lax.rem(y + p.y - 1, p.y) * 2 + c
    ways = (right, left)
    H, S, E, T, F = p.hidden, p.slots, p.ep, p.tok, p.width

    def peer(dz, dx):
        return lax.rem(z_me + dz, p.z) * p.x + lax.rem(x_me + dx, p.x)

    def remote(src, dst, s, r, to):
        return pltpu.make_async_remote_copy(
            src_ref=src, dst_ref=dst, send_sem=s, recv_sem=r, device_id=to, device_id_type=MESH
        )

    def wait_for(ref, sem):
        pltpu.make_async_copy(ref, ref, sem).wait()

    offsets = p.offsets()
    n_peers = len(offsets)
    first_loads = [
        pltpu.make_async_copy(routing_hbm, routing_ref, load_sem.at[4]),
        pltpu.make_async_copy(weight_hbm, weight_ref, load_sem.at[5]),
        pltpu.make_async_copy(tokens_hbm, tokens_ref, load_sem.at[6]),
        pltpu.make_async_copy(cotangent_hbm, cotangent_ref, load_sem.at[7]),
    ]
    loads = [
        pltpu.make_async_copy(gate_hbm, w_gu.at[pl.ds(0, H)], load_sem.at[0]),
        pltpu.make_async_copy(up_hbm, w_gu.at[pl.ds(H, H)], load_sem.at[1]),
        pltpu.make_async_copy(down_hbm, w_dn, load_sem.at[2]),
        pltpu.make_async_copy(
            router_hbm.at[:, pl.ds(pl.multiple_of(t * F, F), F)], r_cols, load_sem.at[3]
        ),
    ]
    for copy in first_loads:
        copy.start()
    barrier = pltpu.get_barrier_semaphore()
    for dz, dx in offsets:
        pl.semaphore_signal(barrier, inc=1, device_id=(peer(dz, dx), t), device_id_type=MESH)
    for j in range(1, p.tp):
        pl.semaphore_signal(
            barrier, inc=1, device_id=(me, lax.rem(t + j, p.tp)), device_id_type=MESH
        )
    for copy in loads:
        copy.start()

    for copy in first_loads:
        copy.wait()
    mark("tables")

    routes = routing_ref[...]
    expert_rows = lax.broadcasted_iota(jnp.int32, (E, T), 0)
    hit = [(expert_rows == routes[k : k + 1, :]).astype(F32) for k in range(2)]
    earlier = (
        lax.broadcasted_iota(jnp.int32, (T, T), 0) < lax.broadcasted_iota(jnp.int32, (T, T), 1)
    ).astype(F32).astype(BF)
    count = dot((hit[0] + hit[1]).astype(BF), earlier)
    pos = [jnp.sum(hit[k] * count, axis=0, keepdims=True) for k in range(2)]
    slot_rows = lax.broadcasted_iota(jnp.int32, (S, T), 0).astype(F32)
    slot = [routes[k : k + 1, :].astype(F32) * p.cap + pos[k] for k in range(2)]
    match = jnp.where((slot_rows == slot[0]) | (slot_rows == slot[1]), 1.0, 0.0)
    tokens = tokens_ref[...]
    match_b = match.astype(BF)
    in_rows = dot(match_b, tokens).reshape(E, p.cap, F)
    tan_rows = dot(match_b, cotangent_ref[...]).reshape(E, p.cap, F)
    send_b[...] = jnp.concatenate([in_rows, tan_rows], axis=1).astype(BF)
    for k in range(2):
        hits[:, k * T : (k + 1) * T] = hit[k]
        places[:, k * T : (k + 1) * T] = pos[k]
    weights = weight_ref[...].astype(F32)
    lane_rows = lax.broadcasted_iota(jnp.int32, (LANES, T), 0)
    lane_slot = (lane_rows & (p.cap - 1)).astype(F32)
    spread = sum(
        dot(hit[k].astype(BF), jnp.where(lane_slot == pos[k], weights[k : k + 1, :], 0.0).astype(BF), 1, 1)
        for k in range(2)
    )
    e_ids = lax.broadcasted_iota(jnp.int32, (E, LANES), 0)
    lane_ids = lax.broadcasted_iota(jnp.int32, (E, LANES), 1)
    dz = z_me - (e_ids >> log2(p.x))
    dz = jnp.where(dz < 0, dz + p.z, dz)
    near = jnp.where(dz == 0, 0, jnp.where(2 * dz <= p.z, 2 * dz - 1, 2 * (p.z - dz)))
    my_place = near * p.x + ((x_me - (e_ids & (p.x - 1))) & (p.x - 1))
    my_lanes = (lane_ids >> log2(p.cap)) == (my_place & (p.per_chunk - 1))
    w_send[...] = jnp.where(my_lanes, spread, 0.0).reshape(E, 1, LANES)

    mark("barrier")
    pl.semaphore_wait(barrier, n_peers + p.tp - 1)
    mark("dispatch")

    for dz, dx in p.early():
        to = peer(dz, dx)
        at = p.place(-dz, -dx)
        remote(send_b.at[to], recv_b.at[at], disp_s, disp_r.at[at // p.per_chunk], (to, t)).start()
    for dz, dx in offsets:
        to = peer(dz, dx)
        at = p.place(-dz, -dx)
        remote(w_send.at[to], w_recv.at[at], wt_s, wt_r, (to, t)).start()
    recv_b[0] = send_b[me]
    w_recv[0] = w_send[me]
    by_token[...] = match.T.astype(BF)

    def move(k, way, a):
        r = (-(k - 1) if way == 0 else k - 1) % p.y
        to_r = (-k if way == 0 else k) % p.y
        copy = remote(
            g.at[r, c, a], g.at[to_r, c, a],
            ag_s.at[0 if k < p.half else 1], ag_r.at[way, k - 1, a], (me, ways[way]),
        )
        copy.start()

    def to_partner(r, a):
        piece = g.at[r, c, a]
        remote(piece, piece, pair_s, pair_r.at[r], (me, partner)).start()

    def from_partner(r):
        wait_for(g.at[r, 1 - c], pair_r.at[r])

    def lanes_of(r):
        return pl.ds(pl.multiple_of(lax.rem(y + r, p.y) * p.slab, p.slab), p.slab)

    def rows_of(r, kind):
        return jnp.concatenate(
            [
                jnp.concatenate([g[r, core, 2 * ch + kind] for ch in range(p.chunks)], axis=0)
                for core in range(2)
            ],
            axis=1,
        )

    def forward(r, first):
        from_partner(r)
        cols = lanes_of(r)
        up = dot(w_gu[:, cols], rows_of(r, 0), 1, 1)
        down = dot(w_dn[:, cols], rows_of(r, 1), 1, 1)
        if first:
            pre[...] = up
            back[...] = down
        else:
            pre[...] += up
            back[...] += down

    def arrive(u):
        mark(f"arrive{u}")
        arrived = p.per_chunk - (1 if u == 0 else 0)
        if arrived:
            wait_for(recv_b.at[pl.ds(0, arrived)], disp_r.at[u])
        both = recv_b[u * p.per_chunk : (u + 1) * p.per_chunk].astype(F32)
        g[0, c, 2 * u] = both[:, : p.cap].reshape(LANES, F).astype(BF)
        g[0, c, 2 * u + 1] = both[:, p.cap :].reshape(LANES, F).astype(BF)
        for a in (2 * u, 2 * u + 1):
            for way in range(2):
                if (u, a) in p.ring_units(1, way):
                    move(1, way, a)
        for a in (2 * u, 2 * u + 1):
            to_partner(0, a)

    def pass_on(k, u):
        mark(f"pass{k}{u}")
        for a in (2 * u, 2 * u + 1):
            for way in range(2):
                if (u, a) not in p.ring_units(k, way):
                    continue
                r = (-k if way == 0 else k) % p.y
                wait_for(g.at[r, c, a], ag_r.at[way, k - 1, a])
                if k < p.half and (u, a) in p.ring_units(k + 1, way):
                    move(k + 1, way, a)
                to_partner(r, a)

    def multiply(k):
        mark(f"multiply{k}")
        for r in sorted({k % p.y, -k % p.y}):
            forward(r, k == 0)

    for kind, k, u in p.gather_order():
        if kind == "arrive":
            arrive(u)
        elif kind == "pass":
            pass_on(k, u)
        else:
            if k == 0:
                for copy in loads:
                    copy.wait()
            multiply(k)
    wait_for(w_recv.at[pl.ds(0, n_peers)], wt_r)
    slot_weight = jnp.concatenate(
        [
            jnp.sum(w_recv[ch * p.per_chunk : (ch + 1) * p.per_chunk], axis=0)
            for ch in range(p.chunks)
        ],
        axis=1,
    )
    mark("hidden")

    part = jnp.zeros((1, S), F32)
    step = 32
    for b in range(0, H, step):
        pg, pu, bp = pre[b : b + step, :], pre[H + b : H + b + step, :], back[b : b + step, :]
        sig = lax.logistic(pg)
        act = pg * sig
        hid = act * pu
        part = part + jnp.sum(hid * bp, axis=0, keepdims=True)
        scaled[b : b + step, :] = (slot_weight * hid).astype(BF)
        hg = slot_weight * bp
        grads[b : b + step, :] = (hg * pu * sig * (1.0 + pg * (1.0 - sig))).astype(BF)
        grads[H + b : H + b + step, :] = (hg * act).astype(BF)
    for ch in range(p.chunks):
        g_part[ch : ch + 1, :] = part[:, ch * LANES : (ch + 1) * LANES]
    g_part[p.chunks :, :] = jnp.zeros((4 - p.chunks, LANES), F32)
    gp_recv[t] = g_part[...]
    grads_t[...] = grads[...].astype(F32).T.astype(BF)

    def slot_block(r):
        block = dot(grads_t[...], w_gu[:, lanes_of(r)])
        low, high = block[:, :F], block[:, F:]
        mine[r] = jnp.where(c == 0, low, high).astype(BF)
        p_send[r] = jnp.where(c == 0, high, low).astype(BF)
        remote(p_send.at[r], p_recv.at[r], ps_s, ps_r.at[r], (me, partner)).start()

    def chip_sum(r, u):
        if r not in ready:
            ready.add(r)
            wait_for(p_recv.at[r], ps_r.at[r])
        rows = pl.ds(u * p.unit_rows, p.unit_rows)
        return mine[r, rows].astype(F32) + p_recv[r, rows].astype(F32)

    def ring_send(way, u, d):
        r = (d if way == 0 else -d) % p.y
        total = chip_sum(r, u)
        longest = p.half if p.long_way(way, u) else p.half - 1
        if d < longest:
            wait_for(rs_r.at[way, u, d], rs_rs.at[way, u, d])
            total = total + rs_r[way, u, d].astype(F32)
        rs_s[way, u, d - 1] = total.astype(BF)
        remote(
            rs_s.at[way, u, d - 1], rs_r.at[way, u, d - 1],
            rs_ss.at[0 if p.long_way(way, u) else 1], rs_rs.at[way, u, d - 1], (me, ways[way]),
        ).start()

    def ring_step(j, long):
        for u in far + near:
            for way in range(2):
                d = p.half - j + (1 if long else 0)
                if p.long_way(way, u) == long and d >= 1:
                    ring_send(way, u, d)

    far, near = (3, 2), (1, 0)
    mark("ring1")
    order = [p.half]
    for d in range(p.half - 1, 0, -1):
        order += [d, p.y - d]
    order.append(0)
    ready = set()
    slot_block(order[0])
    for j in range(1, p.tp):
        remote(g_part, gp_recv.at[t], gp_s, gp_r, (me, lax.rem(t + j, p.tp))).start()
    for r in order[1:4]:
        slot_block(r)
    ring_step(1, True)
    for r in order[4:5]:
        slot_block(r)
    ring_step(1, False)
    for r in order[5:]:
        slot_block(r)

    mark("wgrads1")
    d_acc[...] = jnp.zeros_like(d_acc)

    def weight_grads(r):
        cols = lanes_of(r)
        both = dot(grads[...], rows_of(r, 0))
        dg[:, cols] = both[:H].astype(BF)
        du[:, cols] = both[H:].astype(BF)
        for row, part in enumerate((both[:H], both[H:])):
            square = jnp.sum(part * part, axis=0, keepdims=True)
            for core in range(2):
                sq[2 * lax.rem(y + r, p.y) + core, row : row + 1] = square[:, core * F : (core + 1) * F]
        down = dot(scaled[...], rows_of(r, 1))
        dd[:, cols] = down.astype(BF)
        square = down * down
        d_acc[...] += square[:, :F] + square[:, F:]

    slabs = list(range(p.y))
    per_step = -(-p.y // max(1, p.half - 1)) if p.half > 1 else p.y

    def gate_sum():
        wait_for(gp_recv.at[pl.ds(0, p.tp - 1)], gp_r)
        total = jnp.sum(gp_recv[...], axis=0)
        for ch in range(p.chunks):
            g_send[ch] = total[ch : ch + 1, :]
        for dz, dx in offsets:
            to = peer(dz, dx)
            row = p.place(dz, dx) // p.per_chunk
            remote(g_send.at[row], g_recv.at[me], gc_s, gc_r, (to, t)).start()
        g_recv[me] = g_send[0]

    def send_squares():
        for j in range(1, p.tp):
            to = lax.rem(t + j, p.tp)
            remote(sq.at[to], sq_recv.at[t], sq_s, sq_r, (me, to)).start()
        sq_recv[t] = sq[t]

    for j in range(2, p.half + 1):
        for r in slabs[:per_step]:
            weight_grads(r)
        slabs = slabs[per_step:]
        mark(f"ring{j}")
        ring_step(j, True)
        mark(f"ring{j}b")
        ring_step(j, False)
        if j == 2:
            mark("gate_sum")
            gate_sum()
        mark(f"wgrads{j}")
        if j == p.half - 1 and j > 1:
            for r in slabs:
                weight_grads(r)
            slabs = []
            send_squares()
    for r in slabs:
        weight_grads(r)
    if p.half < 3:
        send_squares()
    if p.half < 2:
        gate_sum()
    mark("last_ring")
    def finish(u):
        total = chip_sum(0, u)
        for way in range(2):
            if p.half > 1 or p.long_way(way, u):
                wait_for(rs_r.at[way, u, 0], rs_rs.at[way, u, 0])
                total = total + rs_r[way, u, 0].astype(F32)
        block[u] = total
        if p.unit_rows % p.cap == 0:
            per = p.unit_rows // p.cap
            c_buf[u * per : (u + 1) * per] = total.reshape(per, p.cap, F).astype(BF)
            sources = range(u * per, (u + 1) * per)
        elif len(block) == p.units:
            whole = jnp.concatenate([block[v] for v in range(p.units)], axis=0)
            c_buf[...] = whole.reshape(E, p.cap, F).astype(BF)
            sources = range(E)
        else:
            sources = ()
        for dz, dx in offsets:
            if p.place(dz, dx) in sources:
                to = peer(dz, dx)
                remote(c_buf.at[p.place(dz, dx)], c_recv.at[me], cb_s, cb_r, (to, t)).start()

    block = {}
    for u in far:
        finish(u)
    mark("gate")
    wait_for(g_recv.at[pl.ds(0, n_peers)], gc_r)
    kept = jnp.where(my_lanes, g_recv[...].reshape(E, LANES), 0.0)
    picked = dot(kept, hits[...], 0, 0, HI)
    lane_twice = jnp.concatenate([lane_slot, lane_slot], axis=1)
    gates = jnp.sum(jnp.where(lane_twice == places[...], picked, 0.0), axis=0, keepdims=True)
    gate = [gates[:, k * T : (k + 1) * T] for k in range(2)]
    for k in range(2):
        gate_out[k : k + 1, :] = gate[k]
    mixed = weights[0:1, :] * gate[0] + weights[1:2, :] * gate[1]
    logit = [weights[k : k + 1, :] * (gate[k] - mixed) for k in range(2)]
    signal = (hits[:, :T] * logit[0] + hits[:, T:] * logit[1]).astype(BF)
    rt_send[...] = dot(signal, tokens).reshape(E, 1, F)
    for dz, dx in offsets:
        to = peer(dz, dx)
        remote(rt_send.at[to], rt_recv.at[me], rt_s, rt_r, (to, t)).start()
    rt_recv[me] = rt_send[me]
    mark("finish")
    for u in near:
        finish(u)
    c_recv[me] = c_buf[0]
    wait_for(sq_recv.at[pl.ds(0, p.tp - 1)], sq_r)
    sq_sum[...] = jnp.sum(sq_recv[...], axis=0) * (1.0 / (H * p.tp))
    for j in range(1, p.tp):
        remote(sq_sum, sq_all.at[t], sa_s, sa_r, (me, lax.rem(t + j, p.tp))).start()
    sq_all[t] = sq_sum[...]
    from_router = dot(signal.astype(F32).T.astype(BF), r_cols[...])
    ones = jnp.ones((8, F), F32)
    dsq_out[...] = dot(ones, d_acc[...], 1, 1, HI)[0:1, :] * (1.0 / p.features)

    mark("token")
    wait_for(c_recv.at[pl.ds(0, n_peers)], cb_r)
    rows = c_recv[...].astype(F32).reshape(S, F).astype(BF)
    token_out[...] = dot(by_token[...], rows) + from_router
    mark("router")
    wait_for(rt_recv.at[pl.ds(0, n_peers)], rt_r)
    router_out[...] = jnp.sum(rt_recv[...], axis=0)
    mark("squares")
    wait_for(sq_all.at[pl.ds(0, p.tp - 1)], sa_r)
    for i in range(p.tp):
        gsq_out[:, i * F : (i + 1) * F] = sq_all[i, 0:1]
        usq_out[:, i * F : (i + 1) * F] = sq_all[i, 1:2]

    mark("sends")
    if p.half > 1:
        wait_for(g.at[pl.ds(0, p.half - 1)], ag_s.at[0])
        wait_for(rs_s.at[0, :, pl.ds(0, p.half - 1)], rs_ss.at[1])
    wait_for(g.at[0, 0], ag_s.at[1])
    wait_for(rs_s.at[0], rs_ss.at[0])
    wait_for(g.at[pl.ds(0, p.half)], pair_s)
    wait_for(p_recv, ps_s)
    wait_for(send_b.at[pl.ds(0, n_peers)], disp_s)
    wait_for(w_send.at[pl.ds(0, n_peers)], wt_s)
    wait_for(gp_recv.at[pl.ds(0, p.tp - 1)], gp_s)
    wait_for(g_recv.at[pl.ds(0, n_peers)], gc_s)
    wait_for(c_recv.at[pl.ds(0, n_peers)], cb_s)
    wait_for(rt_recv.at[pl.ds(0, n_peers)], rt_s)
    wait_for(sq_recv.at[pl.ds(0, p.tp - 1)], sq_s)
    wait_for(sq_all.at[pl.ds(0, p.tp - 1)], sa_s)
    mark(None)


def run(p, routing, weights, tokens, cotangent, gate_t, up_t, down, router_t):
    H, S, E, T, F, D, N = p.hidden, p.slots, p.ep, p.tok, p.width, p.features, p.tp
    vm, hbm = pl.BlockSpec(memory_space=pltpu.VMEM), pl.BlockSpec(memory_space=pltpu.HBM)
    V, dma = pltpu.VMEM, pltpu.SemaphoreType.DMA
    scratch = [
        V((2, T), jnp.int32), V((2, T), BF), V((T, F), BF), V((T, F), BF),
        V((2 * H, D), BF), V((H, D), BF), V((E, F), BF),
        V((E, 2 * p.cap, F), BF), V((E, 2 * p.cap, F), BF),
        V((E, 1, LANES), F32), V((E, 1, LANES), F32),
        V((T, S), BF), V((E, 2 * T), F32), V((1, 2 * T), F32),
        V((p.y, 2, 2 * p.chunks, LANES, F), BF),
        V((2 * H, S), F32), V((H, S), F32), V((2 * H, S), BF), V((S, 2 * H), BF), V((H, S), BF),
        V((4, LANES), F32), V((N, 4, LANES), F32), V((p.chunks, 1, LANES), F32), V((E, 1, LANES), F32),
        V((p.y, S, F), BF), V((p.y, S, F), BF), V((p.y, S, F), BF),
        V((2, p.units, p.half, p.unit_rows, F), BF), V((2, p.units, p.half, p.unit_rows, F), BF),
        V((E, p.cap, F), BF), V((E, p.cap, F), BF),
        V((E, 1, F), F32), V((E, 1, F), F32),
        V((N, 2, F), F32), V((N, 2, F), F32), V((2, F), F32), V((N, 2, F), F32),
        V((H, F), F32),
        dma((8,)), dma, dma((p.chunks,)), dma, dma,
        dma((2,)), dma((2, p.half, 2 * p.chunks)),
        dma, dma((p.y,)),
        dma, dma, dma, dma,
        dma, dma((p.y,)),
        dma((2,)), dma((2, p.units, p.half)),
        dma, dma, dma, dma, dma, dma, dma, dma,
    ]
    shape = jax.ShapeDtypeStruct
    shapes = (
        shape((T, F), F32), shape((2, T), F32),
        shape((H, D), BF), shape((H, D), BF), shape((H, D), BF),
        shape((1, F), F32), shape((1, D), F32), shape((1, D), F32), shape((1, H), F32),
    )
    results = pl.pallas_call(
        functools.partial(kernel, p),
        out_shape=shapes,
        in_specs=[hbm] * 8,
        out_specs=(vm,) * len(shapes),
        scratch_shapes=scratch,
        compiler_params=pltpu.CompilerParams(
            collective_id=0, has_side_effects=True, vmem_limit_bytes=40 << 20
        ),
        name="expert_backward",
    )(*(
        pltpu.with_memory_space_constraint(a, pltpu.HBM)
        for a in (routing, weights, tokens, cotangent, gate_t, up_t, down, router_t)
    ))
    return pl.pallas_call(
        store,
        out_shape=shapes,
        in_specs=[vm] * len(shapes),
        out_specs=(hbm,) * len(shapes),
        scratch_shapes=[dma((len(shapes),))],
        compiler_params=pltpu.CompilerParams(vmem_limit_bytes=1 << 20),
        name="store_results",
    )(*results)


def store(*refs):
    n = len(refs) // 2
    copies = [pltpu.make_async_copy(refs[i], refs[n + i], refs[-1].at[i]) for i in range(n)]
    for copy in copies:
        copy.start()
    for copy in copies:
        copy.wait()


def shards(tokens, routing, gate_weights, cotangent, expert_gate, expert_up, expert_down, router):
    tok, width = tokens.shape
    n_ep, n_tp = lax.axis_size("ep"), lax.axis_size("tp")
    experts = router.shape[1]
    cap = 3 * routing.shape[1] * tok // (2 * experts)
    p = Plan(n_ep, n_tp, tok, width, expert_gate.shape[2], width * n_tp, cap)
    out = run(
        p, routing.T, gate_weights.T, tokens, cotangent,
        expert_gate[0].T, expert_up[0].T, expert_down[0], router.T,
    )
    token_grad, gate_grad, dgate, dup, ddown, router_grad, gsq, usq, dsq = out
    return (
        token_grad, gate_grad.T, dgate.T[None], dup.T[None], ddown[None], router_grad, gsq, usq, dsq,
    )


def solution(mesh):
    in_specs = (
        P("ep", "tp"),
        P("ep", None),
        P("ep", None),
        P("ep", "tp"),
        P("ep", None, "tp"),
        P("ep", None, "tp"),
        P("ep", "tp", None),
        P(),
    )
    out_specs = (
        P("ep", "tp"),
        P("ep", None),
        P("ep", None, "tp"),
        P("ep", None, "tp"),
        P("ep", "tp", None),
        P("ep", "tp"),
        P("ep", None),
        P("ep", None),
        P("ep", "tp"),
    )
    return jax.shard_map(shards, mesh=mesh, in_specs=in_specs, out_specs=out_specs, check_vma=False)
```

```python
import functools

import jax
import jax.numpy as jnp
from jax import lax
from jax.experimental import pallas as pl
from jax.experimental.pallas import tpu as pltpu
from jax.sharding import PartitionSpec as P

MESH = pl.DeviceIdType.MESH
BF = jnp.bfloat16
F32 = jnp.float32
LANES = 128
HI = lax.Precision.HIGHEST


def dot(a, b, ca=1, cb=0, precision=None):
    return lax.dot_general(
        a, b, (((ca,), (cb,)), ((), ())), precision=precision, preferred_element_type=F32
    )


def log2(n):
    return n.bit_length() - 1


class Marks:
    def __init__(self):
        self.scope = None

    def __call__(self, name):
        if self.scope is not None:
            self.scope.__exit__(None, None, None)
        self.scope = jax.named_scope(name) if name else None
        if name:
            self.scope.__enter__()


class Plan:
    def __init__(self, n_ep, n_tp, tok, width, hidden, features, cap):
        self.ep, self.tp, self.tok, self.width = n_ep, n_tp, tok, width
        self.hidden, self.features, self.cap = hidden, features, cap
        self.x = 4 if n_ep % 4 == 0 else 1
        self.z = n_ep // self.x
        self.y = n_tp // 2
        self.half = self.y // 2
        self.slots = n_ep * cap
        self.chunks = self.slots // LANES
        self.per_chunk = LANES // cap
        self.units = 6
        self.unit_rows = self.slots // self.units
        self.slab = 2 * width

    def near(self, dz):
        dz %= self.z
        if dz == 0:
            return 0
        return 2 * dz - 1 if 2 * dz <= self.z else 2 * (self.z - dz)

    def place(self, dz, dx):
        return self.near(dz) * self.x + dx % self.x

    def offsets(self):
        found = [(dz, dx) for dz in range(self.z) for dx in range(self.x) if (dz, dx) != (0, 0)]

        def hops(o):
            return min(o[0], self.z - o[0]) + min(o[1], self.x - o[1])

        return sorted(found, key=lambda o: (-hops(o), o[1], o[0]))

    def ring_units(self, k, way):
        kinds = (way,) if k == self.half else (0, 1)
        return [(u, 2 * u + kind) for u in range(self.chunks) for kind in kinds]

    def early(self):
        return sorted(self.offsets(), key=lambda o: self.place(-o[0], -o[1]) // self.per_chunk)

    def gather_order(self):
        if self.half == 4 and self.chunks == 3:
            a, p, m = "arrive", "pass", "multiply"
            return (
                (a, 0, 0), (a, 0, 1), (p, 1, 0), (a, 0, 2), (p, 1, 1), (p, 2, 0), (p, 1, 2),
                (p, 2, 1), (m, 0, 0), (p, 2, 2), (p, 3, 0), (m, 1, 0), (p, 3, 1), (p, 3, 2),
                (p, 4, 0), (m, 2, 0), (p, 4, 1), (p, 4, 2), (m, 3, 0), (m, 4, 0),
            )
        out = [("arrive", 0, u) for u in range(self.chunks)] + [("multiply", 0, 0)]
        for k in range(1, self.half + 1):
            out += [("pass", k, u) for u in range(self.chunks)] + [("multiply", k, 0)]
        return out

    def long_way(self, way, u):
        return u % 2 == way


def kernel(
    p,
    routing_hbm, weight_hbm, tokens_hbm, cotangent_hbm, gate_hbm, up_hbm, down_hbm, router_hbm,
    token_out, gate_out, dg, du, dd, router_out, gsq_out, usq_out, dsq_out,
    routing_ref, weight_ref, tokens_ref, cotangent_ref,
    w_gu, w_dn, r_cols, send_b, recv_b, w_send, w_recv, by_token, hits, places,
    g, pre, back, grads, grads_t, scaled, g_part, gp_recv, g_send, g_recv,
    mine, p_send, p_recv, rs_s, rs_r, c_buf, c_recv, rt_send, rt_recv, sq, sq_recv, sq_sum, sq_all,
    d_acc,
    load_sem, disp_s, disp_r, wt_s, wt_r, ag_s, ag_r, pair_s, pair_r, gp_s, gp_r, gc_s, gc_r,
    ps_s, ps_r, rs_ss, rs_rs, cb_s, cb_r, rt_s, rt_r, sq_s, sq_r, sa_s, sa_r,
):
    mark = Marks()
    mark("start")
    me = lax.axis_index("ep")
    t = lax.axis_index("tp")
    y, c = lax.div(t, 2), lax.rem(t, 2)
    z_me, x_me = lax.div(me, p.x), lax.rem(me, p.x)
    partner = t + 1 - 2 * c
    right = lax.rem(y + 1, p.y) * 2 + c
    left = lax.rem(y + p.y - 1, p.y) * 2 + c
    ways = (right, left)
    other_ways = (right + 1 - 2 * c, left + 1 - 2 * c)
    H, S, E, T, F = p.hidden, p.slots, p.ep, p.tok, p.width

    def peer(dz, dx):
        return lax.rem(z_me + dz, p.z) * p.x + lax.rem(x_me + dx, p.x)

    def remote(src, dst, s, r, to):
        return pltpu.make_async_remote_copy(
            src_ref=src, dst_ref=dst, send_sem=s, recv_sem=r, device_id=to, device_id_type=MESH
        )

    def wait_for(ref, sem):
        pltpu.make_async_copy(ref, ref, sem).wait()

    offsets = p.offsets()
    n_peers = len(offsets)
    first_loads = [
        pltpu.make_async_copy(routing_hbm, routing_ref, load_sem.at[4]),
        pltpu.make_async_copy(weight_hbm, weight_ref, load_sem.at[5]),
        pltpu.make_async_copy(tokens_hbm, tokens_ref, load_sem.at[6]),
        pltpu.make_async_copy(cotangent_hbm, cotangent_ref, load_sem.at[7]),
    ]
    loads = [
        pltpu.make_async_copy(gate_hbm, w_gu.at[pl.ds(0, H)], load_sem.at[0]),
        pltpu.make_async_copy(up_hbm, w_gu.at[pl.ds(H, H)], load_sem.at[1]),
        pltpu.make_async_copy(down_hbm, w_dn, load_sem.at[2]),
        pltpu.make_async_copy(
            router_hbm.at[:, pl.ds(pl.multiple_of(t * F, F), F)], r_cols, load_sem.at[3]
        ),
    ]
    for copy in first_loads:
        copy.start()
    barrier = pltpu.get_barrier_semaphore()
    for dz, dx in offsets:
        pl.semaphore_signal(barrier, inc=1, device_id=(peer(dz, dx), t), device_id_type=MESH)
    for j in range(1, p.tp):
        pl.semaphore_signal(
            barrier, inc=1, device_id=(me, lax.rem(t + j, p.tp)), device_id_type=MESH
        )
    for copy in loads:
        copy.start()

    for copy in first_loads:
        copy.wait()
    mark("tables")

    routes = routing_ref[...]
    expert_rows = lax.broadcasted_iota(jnp.int32, (E, T), 0)
    hit = [(expert_rows == routes[k : k + 1, :]).astype(F32) for k in range(2)]
    earlier = (
        lax.broadcasted_iota(jnp.int32, (T, T), 0) < lax.broadcasted_iota(jnp.int32, (T, T), 1)
    ).astype(F32).astype(BF)
    count = dot((hit[0] + hit[1]).astype(BF), earlier)
    pos = [jnp.sum(hit[k] * count, axis=0, keepdims=True) for k in range(2)]
    slot_rows = lax.broadcasted_iota(jnp.int32, (S, T), 0).astype(F32)
    slot = [routes[k : k + 1, :].astype(F32) * p.cap + pos[k] for k in range(2)]
    match = jnp.where((slot_rows == slot[0]) | (slot_rows == slot[1]), 1.0, 0.0)
    tokens = tokens_ref[...]
    match_b = match.astype(BF)
    in_rows = dot(match_b, tokens).reshape(E, p.cap, F)
    tan_rows = dot(match_b, cotangent_ref[...]).reshape(E, p.cap, F)
    send_b[...] = jnp.concatenate([in_rows, tan_rows], axis=1).astype(BF)
    for k in range(2):
        hits[:, k * T : (k + 1) * T] = hit[k]
        places[:, k * T : (k + 1) * T] = pos[k]
    weights = weight_ref[...].astype(F32)
    lane_rows = lax.broadcasted_iota(jnp.int32, (LANES, T), 0)
    lane_slot = (lane_rows & (p.cap - 1)).astype(F32)
    spread = sum(
        dot(hit[k].astype(BF), jnp.where(lane_slot == pos[k], weights[k : k + 1, :], 0.0).astype(BF), 1, 1)
        for k in range(2)
    )
    e_ids = lax.broadcasted_iota(jnp.int32, (E, LANES), 0)
    lane_ids = lax.broadcasted_iota(jnp.int32, (E, LANES), 1)
    dz = z_me - (e_ids >> log2(p.x))
    dz = jnp.where(dz < 0, dz + p.z, dz)
    near = jnp.where(dz == 0, 0, jnp.where(2 * dz <= p.z, 2 * dz - 1, 2 * (p.z - dz)))
    my_place = near * p.x + ((x_me - (e_ids & (p.x - 1))) & (p.x - 1))
    my_lanes = (lane_ids >> log2(p.cap)) == (my_place & (p.per_chunk - 1))
    w_send[...] = jnp.where(my_lanes, spread, 0.0).reshape(E, 1, LANES)

    mark("barrier")
    pl.semaphore_wait(barrier, n_peers + p.tp - 1)
    mark("dispatch")

    for dz, dx in p.early():
        to = peer(dz, dx)
        at = p.place(-dz, -dx)
        remote(send_b.at[to], recv_b.at[at], disp_s, disp_r.at[at // p.per_chunk], (to, t)).start()
    recv_b[0] = send_b[me]
    by_token[...] = match.T.astype(BF)

    def move(k, way, a):
        r = (-(k - 1) if way == 0 else k - 1) % p.y
        to_r = (-k if way == 0 else k) % p.y
        copy = remote(
            g.at[r, c, a], g.at[to_r, c, a],
            ag_s.at[0 if k < p.half else 1], ag_r.at[way, k - 1, a], (me, ways[way]),
        )
        copy.start()

    def both_cores(k, a):
        return k == p.half and k > 1 and a // 2 == p.chunks - 1

    def to_partner(r, a):
        piece = g.at[r, c, a]
        remote(piece, piece, pair_s, pair_r.at[r], (me, partner)).start()

    def from_partner(r):
        wait_for(g.at[r, 1 - c], pair_r.at[r])

    def lanes_of(r):
        return pl.ds(pl.multiple_of(lax.rem(y + r, p.y) * p.slab, p.slab), p.slab)

    def rows_of(r, kind):
        return jnp.concatenate(
            [
                jnp.concatenate([g[r, core, 2 * ch + kind] for ch in range(p.chunks)], axis=0)
                for core in range(2)
            ],
            axis=1,
        )

    def forward(r, first):
        from_partner(r)
        cols = lanes_of(r)
        up = dot(w_gu[:, cols], rows_of(r, 0), 1, 1)
        down = dot(w_dn[:, cols], rows_of(r, 1), 1, 1)
        if first:
            pre[...] = up
            back[...] = down
        else:
            pre[...] += up
            back[...] += down

    def arrive(u):
        mark(f"arrive{u}")
        arrived = p.per_chunk - (1 if u == 0 else 0)
        if arrived:
            wait_for(recv_b.at[pl.ds(0, arrived)], disp_r.at[u])
        both = recv_b[u * p.per_chunk : (u + 1) * p.per_chunk].astype(F32)
        g[0, c, 2 * u] = both[:, : p.cap].reshape(LANES, F).astype(BF)
        g[0, c, 2 * u + 1] = both[:, p.cap :].reshape(LANES, F).astype(BF)
        for a in (2 * u, 2 * u + 1):
            for way in range(2):
                if (u, a) in p.ring_units(1, way):
                    move(1, way, a)
        for a in (2 * u, 2 * u + 1):
            to_partner(0, a)

    def send_weights():
        for dz, dx in offsets:
            to = peer(dz, dx)
            at = p.place(-dz, -dx)
            remote(w_send.at[to], w_recv.at[at], wt_s, wt_r, (to, t)).start()
        w_recv[0] = w_send[me]

    def pass_on(k, u):
        mark(f"pass{k}{u}")
        for a in (2 * u, 2 * u + 1):
            for way in range(2):
                if (u, a) not in p.ring_units(k, way):
                    continue
                r = (-k if way == 0 else k) % p.y
                wait_for(g.at[r, c, a], ag_r.at[way, k - 1, a])
                if k < p.half and (u, a) in p.ring_units(k + 1, way):
                    move(k + 1, way, a)
                    if both_cores(k + 1, a):
                        remote(
                            g.at[r, c, a], g.at[p.half, c, a],
                            pair_s, pair_r.at[p.half], (me, other_ways[way]),
                        ).start()
                if not both_cores(k, a):
                    to_partner(r, a)

    def multiply(k):
        mark(f"multiply{k}")
        for r in sorted({k % p.y, -k % p.y}):
            forward(r, k == 0)

    for kind, k, u in p.gather_order():
        if kind == "arrive":
            arrive(u)
            if u == p.chunks - 1:
                send_weights()
        elif kind == "pass":
            pass_on(k, u)
        else:
            if k == 0:
                for copy in loads:
                    copy.wait()
            multiply(k)
    wait_for(w_recv.at[pl.ds(0, n_peers)], wt_r)
    slot_weight = jnp.concatenate(
        [
            jnp.sum(w_recv[ch * p.per_chunk : (ch + 1) * p.per_chunk], axis=0)
            for ch in range(p.chunks)
        ],
        axis=1,
    )
    mark("hidden")

    part = jnp.zeros((1, S), F32)
    step = 32
    for b in range(0, H, step):
        pg, pu, bp = pre[b : b + step, :], pre[H + b : H + b + step, :], back[b : b + step, :]
        sig = lax.logistic(pg)
        act = pg * sig
        hid = act * pu
        part = part + jnp.sum(hid * bp, axis=0, keepdims=True)
        scaled[b : b + step, :] = (slot_weight * hid).astype(BF)
        hg = slot_weight * bp
        grads[b : b + step, :] = (hg * pu * sig * (1.0 + pg * (1.0 - sig))).astype(BF)
        grads[H + b : H + b + step, :] = (hg * act).astype(BF)
    for ch in range(p.chunks):
        g_part[ch : ch + 1, :] = part[:, ch * LANES : (ch + 1) * LANES]
    g_part[p.chunks :, :] = jnp.zeros((4 - p.chunks, LANES), F32)
    gp_recv[t] = g_part[...]
    grads_t[...] = grads[...].astype(F32).T.astype(BF)

    def slot_block(r):
        block = dot(grads_t[...], w_gu[:, lanes_of(r)])
        low, high = block[:, :F], block[:, F:]
        mine[r] = jnp.where(c == 0, low, high).astype(BF)
        p_send[r] = jnp.where(c == 0, high, low).astype(BF)
        remote(p_send.at[r], p_recv.at[r], ps_s, ps_r.at[r], (me, partner)).start()

    def chip_sum(r, u):
        if r not in ready:
            ready.add(r)
            wait_for(p_recv.at[r], ps_r.at[r])
        rows = pl.ds(u * p.unit_rows, p.unit_rows)
        return mine[r, rows].astype(F32) + p_recv[r, rows].astype(F32)

    def ring_send(way, u, d):
        r = (d if way == 0 else -d) % p.y
        total = chip_sum(r, u)
        longest = p.half if p.long_way(way, u) else p.half - 1
        if d < longest:
            wait_for(rs_r.at[way, u, d], rs_rs.at[way, u, d])
            total = total + rs_r[way, u, d].astype(F32)
        rs_s[way, u, d - 1] = total.astype(BF)
        remote(
            rs_s.at[way, u, d - 1], rs_r.at[way, u, d - 1],
            rs_ss.at[0 if p.long_way(way, u) else 1], rs_rs.at[way, u, d - 1], (me, ways[way]),
        ).start()

    def ring_step(j, long):
        for u in far + near:
            for way in range(2):
                d = p.half - j + (1 if long else 0)
                if p.long_way(way, u) == long and d >= 1:
                    ring_send(way, u, d)

    backward = tuple(range(p.units))[::-1]
    far, near = backward[: p.units // 2], backward[p.units // 2 :]
    mark("ring1")
    order = [p.half]
    for d in range(p.half - 1, 0, -1):
        order += [d, p.y - d]
    order.append(0)
    ready = set()
    slot_block(order[0])
    for j in range(1, p.tp):
        remote(g_part, gp_recv.at[t], gp_s, gp_r, (me, lax.rem(t + j, p.tp))).start()
    for r in order[1:4]:
        slot_block(r)
    ring_step(1, True)
    for r in order[4:5]:
        slot_block(r)
    ring_step(1, False)
    for r in order[5:]:
        slot_block(r)

    mark("wgrads1")
    d_acc[...] = jnp.zeros_like(d_acc)

    def weight_grads(r):
        cols = lanes_of(r)
        both = dot(grads[...], rows_of(r, 0))
        dg[:, cols] = both[:H].astype(BF)
        du[:, cols] = both[H:].astype(BF)
        for row, part in enumerate((both[:H], both[H:])):
            square = jnp.sum(part * part, axis=0, keepdims=True)
            for core in range(2):
                sq[2 * lax.rem(y + r, p.y) + core, row : row + 1] = square[:, core * F : (core + 1) * F]
        down = dot(scaled[...], rows_of(r, 1))
        dd[:, cols] = down.astype(BF)
        square = down * down
        d_acc[...] += square[:, :F] + square[:, F:]

    slabs = list(range(p.y))

    def gate_sum():
        wait_for(gp_recv.at[pl.ds(0, p.tp - 1)], gp_r)
        total = jnp.sum(gp_recv[...], axis=0)
        for ch in range(p.chunks):
            g_send[ch] = total[ch : ch + 1, :]
        for dz, dx in offsets:
            to = peer(dz, dx)
            row = p.place(dz, dx) // p.per_chunk
            remote(g_send.at[row], g_recv.at[me], gc_s, gc_r, (to, t)).start()
        g_recv[me] = g_send[0]

    def send_squares():
        for j in range(1, p.tp):
            to = lax.rem(t + j, p.tp)
            remote(sq.at[to], sq_recv.at[t], sq_s, sq_r, (me, to)).start()
        sq_recv[t] = sq[t]

    counts = {1: 3, 2: 2, 3: 3} if p.half == 4 else {}
    for r in slabs[: counts.get(1, 0)]:
        weight_grads(r)
    slabs = slabs[counts.get(1, 0) :]
    for j in range(2, p.half + 1):
        mark(f"ring{j}")
        ring_step(j, True)
        if j == 2:
            mark("gate_sum")
            gate_sum()
        mark(f"ring{j}b")
        ring_step(j, False)
        mark(f"wgrads{j}")
        for r in slabs[: counts.get(j, 0)]:
            weight_grads(r)
        slabs = slabs[counts.get(j, 0) :]
        if j == max(counts, default=0):
            send_squares()
    if p.half < 2:
        gate_sum()
    for r in slabs:
        weight_grads(r)
    if not counts:
        send_squares()
    mark("last_ring")
    def finish(u):
        total = chip_sum(0, u)
        for way in range(2):
            if p.half > 1 or p.long_way(way, u):
                wait_for(rs_r.at[way, u, 0], rs_rs.at[way, u, 0])
                total = total + rs_r[way, u, 0].astype(F32)
        block[u] = total
        if p.unit_rows % p.cap == 0:
            per = p.unit_rows // p.cap
            c_buf[u * per : (u + 1) * per] = total.reshape(per, p.cap, F).astype(BF)
            sources = range(u * per, (u + 1) * per)
        elif len(block) == p.units:
            whole = jnp.concatenate([block[v] for v in range(p.units)], axis=0)
            c_buf[...] = whole.reshape(E, p.cap, F).astype(BF)
            sources = range(E)
        else:
            sources = ()
        for dz, dx in offsets:
            if p.place(dz, dx) in sources:
                to = peer(dz, dx)
                remote(c_buf.at[p.place(dz, dx)], c_recv.at[me], cb_s, cb_r, (to, t)).start()

    block = {}
    for u in far:
        finish(u)
    mark("gate")
    wait_for(g_recv.at[pl.ds(0, n_peers)], gc_r)
    kept = jnp.where(my_lanes, g_recv[...].reshape(E, LANES), 0.0)
    picked = dot(kept, hits[...], 0, 0, HI)
    lane_twice = jnp.concatenate([lane_slot, lane_slot], axis=1)
    gates = jnp.sum(jnp.where(lane_twice == places[...], picked, 0.0), axis=0, keepdims=True)
    gate = [gates[:, k * T : (k + 1) * T] for k in range(2)]
    for k in range(2):
        gate_out[k : k + 1, :] = gate[k]
    mixed = weights[0:1, :] * gate[0] + weights[1:2, :] * gate[1]
    logit = [weights[k : k + 1, :] * (gate[k] - mixed) for k in range(2)]
    signal = (hits[:, :T] * logit[0] + hits[:, T:] * logit[1]).astype(BF)
    rt_send[...] = dot(signal, tokens).reshape(E, 1, F)
    for dz, dx in offsets:
        to = peer(dz, dx)
        remote(rt_send.at[to], rt_recv.at[me], rt_s, rt_r, (to, t)).start()
    rt_recv[me] = rt_send[me]
    mark("finish")
    for u in near:
        finish(u)
    c_recv[me] = c_buf[0]
    from_router = dot(signal.astype(F32).T.astype(BF), r_cols[...])
    ones = jnp.ones((8, F), F32)
    dsq_out[...] = dot(ones, d_acc[...], 1, 1, HI)[0:1, :] * (1.0 / p.features)

    wait_for(sq_recv.at[pl.ds(0, p.tp - 1)], sq_r)
    sq_sum[...] = jnp.sum(sq_recv[...], axis=0) * (1.0 / (H * p.tp))
    for j in range(1, p.tp):
        remote(sq_sum, sq_all.at[t], sa_s, sa_r, (me, lax.rem(t + j, p.tp))).start()
    sq_all[t] = sq_sum[...]
    mark("token")
    wait_for(c_recv.at[pl.ds(0, n_peers)], cb_r)
    rows = c_recv[...].astype(F32).reshape(S, F).astype(BF)
    token_out[...] = dot(by_token[...], rows) + from_router
    mark("router")
    wait_for(rt_recv.at[pl.ds(0, n_peers)], rt_r)
    router_out[...] = jnp.sum(rt_recv[...], axis=0)
    mark("squares")
    wait_for(sq_all.at[pl.ds(0, p.tp - 1)], sa_r)
    for i in range(p.tp):
        gsq_out[:, i * F : (i + 1) * F] = sq_all[i, 0:1]
        usq_out[:, i * F : (i + 1) * F] = sq_all[i, 1:2]

    mark("sends")
    if p.half > 1:
        wait_for(g.at[pl.ds(0, p.half - 1)], ag_s.at[0])
        wait_for(rs_s.at[0, :, pl.ds(0, p.half - 1)], rs_ss.at[1])
    wait_for(g.at[0, 0], ag_s.at[1])
    wait_for(rs_s.at[0], rs_ss.at[0])
    wait_for(g.at[pl.ds(0, p.half)], pair_s)
    wait_for(p_recv, ps_s)
    wait_for(send_b.at[pl.ds(0, n_peers)], disp_s)
    wait_for(w_send.at[pl.ds(0, n_peers)], wt_s)
    wait_for(gp_recv.at[pl.ds(0, p.tp - 1)], gp_s)
    wait_for(g_recv.at[pl.ds(0, n_peers)], gc_s)
    wait_for(c_recv.at[pl.ds(0, n_peers)], cb_s)
    wait_for(rt_recv.at[pl.ds(0, n_peers)], rt_s)
    wait_for(sq_recv.at[pl.ds(0, p.tp - 1)], sq_s)
    wait_for(sq_all.at[pl.ds(0, p.tp - 1)], sa_s)
    mark(None)


def run(p, routing, weights, tokens, cotangent, gate_t, up_t, down, router_t):
    H, S, E, T, F, D, N = p.hidden, p.slots, p.ep, p.tok, p.width, p.features, p.tp
    vm, hbm = pl.BlockSpec(memory_space=pltpu.VMEM), pl.BlockSpec(memory_space=pltpu.HBM)
    V, dma = pltpu.VMEM, pltpu.SemaphoreType.DMA
    scratch = [
        V((2, T), jnp.int32), V((2, T), BF), V((T, F), BF), V((T, F), BF),
        V((2 * H, D), BF), V((H, D), BF), V((E, F), BF),
        V((E, 2 * p.cap, F), BF), V((E, 2 * p.cap, F), BF),
        V((E, 1, LANES), F32), V((E, 1, LANES), F32),
        V((T, S), BF), V((E, 2 * T), F32), V((1, 2 * T), F32),
        V((p.y, 2, 2 * p.chunks, LANES, F), BF),
        V((2 * H, S), F32), V((H, S), F32), V((2 * H, S), BF), V((S, 2 * H), BF), V((H, S), BF),
        V((4, LANES), F32), V((N, 4, LANES), F32), V((p.chunks, 1, LANES), F32), V((E, 1, LANES), F32),
        V((p.y, S, F), BF), V((p.y, S, F), BF), V((p.y, S, F), BF),
        V((2, p.units, p.half, p.unit_rows, F), BF), V((2, p.units, p.half, p.unit_rows, F), BF),
        V((E, p.cap, F), BF), V((E, p.cap, F), BF),
        V((E, 1, F), F32), V((E, 1, F), F32),
        V((N, 2, F), F32), V((N, 2, F), F32), V((2, F), F32), V((N, 2, F), F32),
        V((H, F), F32),
        dma((8,)), dma, dma((p.chunks,)), dma, dma,
        dma((2,)), dma((2, p.half, 2 * p.chunks)),
        dma, dma((p.y,)),
        dma, dma, dma, dma,
        dma, dma((p.y,)),
        dma((2,)), dma((2, p.units, p.half)),
        dma, dma, dma, dma, dma, dma, dma, dma,
    ]
    shape = jax.ShapeDtypeStruct
    shapes = (
        shape((T, F), F32), shape((2, T), F32),
        shape((H, D), BF), shape((H, D), BF), shape((H, D), BF),
        shape((1, F), F32), shape((1, D), F32), shape((1, D), F32), shape((1, H), F32),
    )
    results = pl.pallas_call(
        functools.partial(kernel, p),
        out_shape=shapes,
        in_specs=[hbm] * 8,
        out_specs=(vm,) * len(shapes),
        scratch_shapes=scratch,
        compiler_params=pltpu.CompilerParams(
            collective_id=0, has_side_effects=True, vmem_limit_bytes=40 << 20
        ),
        name="expert_backward",
    )(*(
        pltpu.with_memory_space_constraint(a, pltpu.HBM)
        for a in (routing, weights, tokens, cotangent, gate_t, up_t, down, router_t)
    ))
    return pl.pallas_call(
        store,
        out_shape=shapes,
        in_specs=[vm] * len(shapes),
        out_specs=(hbm,) * len(shapes),
        scratch_shapes=[dma((len(shapes),))],
        compiler_params=pltpu.CompilerParams(vmem_limit_bytes=1 << 20),
        name="store_results",
    )(*results)


def store(*refs):
    n = len(refs) // 2
    copies = [pltpu.make_async_copy(refs[i], refs[n + i], refs[-1].at[i]) for i in range(n)]
    for copy in copies:
        copy.start()
    for copy in copies:
        copy.wait()


def shards(tokens, routing, gate_weights, cotangent, expert_gate, expert_up, expert_down, router):
    tok, width = tokens.shape
    n_ep, n_tp = lax.axis_size("ep"), lax.axis_size("tp")
    experts = router.shape[1]
    cap = 3 * routing.shape[1] * tok // (2 * experts)
    p = Plan(n_ep, n_tp, tok, width, expert_gate.shape[2], width * n_tp, cap)
    out = run(
        p, routing.T, gate_weights.T, tokens, cotangent,
        expert_gate[0].T, expert_up[0].T, expert_down[0], router.T,
    )
    token_grad, gate_grad, dgate, dup, ddown, router_grad, gsq, usq, dsq = out
    return (
        token_grad, gate_grad.T, dgate.T[None], dup.T[None], ddown[None], router_grad, gsq, usq, dsq,
    )


def solution(mesh):
    in_specs = (
        P("ep", "tp"),
        P("ep", None),
        P("ep", None),
        P("ep", "tp"),
        P("ep", None, "tp"),
        P("ep", None, "tp"),
        P("ep", "tp", None),
        P(),
    )
    out_specs = (
        P("ep", "tp"),
        P("ep", None),
        P("ep", None, "tp"),
        P("ep", None, "tp"),
        P("ep", "tp", None),
        P("ep", "tp"),
        P("ep", None),
        P("ep", None),
        P("ep", "tp"),
    )
    return jax.shard_map(shards, mesh=mesh, in_specs=in_specs, out_specs=out_specs, check_vma=False)
```
